32 devices in a mesh: sp: 8 (over z, core), tp: 4 (over y, x).
Axes of the slice: x: 2, y: 2, z: 4, core: 2. Of those that a mesh axis runs over, the one named last changes fastest.
Arguments:
- queries: bfloat16 [4096, 1024], P('sp', 'tp'), may hold values from -20 to 20
- key_vectors: bfloat16 [4096, 1024], P('sp', 'tp'), may hold values from -20 to 20
- value_vectors: bfloat16 [4096, 1024], P('sp', 'tp'), may hold values from -6 to 6
- log_gate_sums: float32 [4096, 16], P('sp', 'tp'), may hold values from -588 to 0, as said below
- residual: bfloat16 [4096, 2048], P('sp', 'tp'), may hold values from -24 to 24
- out_weight: bfloat16 [1024, 2048], P(None, 'tp'), may hold values from -0.75 to 0.75
- norm_gain: bfloat16 [2048], replicated, may hold values from 0.099609375 to 1.8984375
- routes: int32 [4096, 2], P('sp'), may hold values from 0 to 31, all different within a row; in each aligned block of 512 rows (0 to 511, 512 to 1023, ...) at most 40 rows name the same one
- route_weight: float32 [4096, 2], P('sp'), may hold values from 0.5 to 1.5
- expert_gate: bfloat16 [32, 2048, 512], P('sp', None, 'tp'), may hold values from -0.125 to 0.125
- expert_up: bfloat16 [32, 2048, 512], P('sp', None, 'tp'), may hold values from -0.125 to 0.125
- expert_down: bfloat16 [32, 512, 2048], P('sp', None, 'tp'), may hold values from -0.25 to 0.25
- shared_gate: bfloat16 [2048, 512], P(None, 'tp'), may hold values from -0.125 to 0.125
- shared_up: bfloat16 [2048, 512], P(None, 'tp'), may hold values from -0.125 to 0.125
- shared_down: bfloat16 [512, 2048], P(None, 'tp'), may hold values from -0.25 to 0.25
Outputs:
- layer_out: bfloat16 [4096, 2048], P('sp', 'tp')
The draws below stay inside these ranges and needn't reach their ends.
Inputs may be any that keep to these rules, and one draw needn't show every extreme that they name: `log_gate_sums`: for each head the values do not rise along the positions. `routes`: each row names 2 different experts; among the rows of one index of sp no expert is named by more than 40 rows, a bound that some block reaches.
All inputs are finite; a program needn't handle non-finite values.
Results may differ from the reference program's by a relative error of at most 0.014.
Values may be sent and summed in bfloat16 or wider, within the bound.
No kernel may reach another device: no remote copies, remote signals or barrier semaphores. Data moves between devices by JAX's collectives and lax.ppermute only.
A program may use at most 64 MiB of HBM per device.

```python
import math
import jax
import jax.numpy as jnp
import numpy as np
from jax import lax

D = 2048
HEAD_TOTAL = 16
HDIM = 64
EF = 512
SH = 512
TOPK = 2
TOK_DEV = 512
TOKEN_TOTAL = 4096
EXPERTS = 32
CAP = 40
N_SP = 8


def attention_pair(key):
    base_key = jax.random.fold_in(key, 11)
    key_query, key_keys = jax.random.split(base_key, 2)
    width = HEAD_TOTAL * HDIM
    query_draw = 1.5 * jax.random.normal(key_query, (TOKEN_TOTAL, width), jnp.float32)
    key_draw = 1.5 * jax.random.normal(key_keys, (TOKEN_TOTAL, width), jnp.float32)
    return (jnp.clip(query_draw, -20.0, 20.0), jnp.clip(key_draw, -20.0, 20.0))


def draw_queries(key, part):
    return attention_pair(key)[0].astype(jnp.bfloat16)


def draw_key_vectors(key, part):
    return attention_pair(key)[1].astype(jnp.bfloat16)


def draw_log_gate_sums(key, part):
    key_a, key_b, key_c, random_key_fourth, random_key_fifth = jax.random.split(jax.random.fold_in(key, 23), 5)
    keep_share = 0.5
    slower_decay_heads = jax.random.bernoulli(key_a, keep_share, (HEAD_TOTAL,))
    rate = jnp.where(slower_decay_heads, 0.4 / TOKEN_TOTAL, 1.0 / 40.0)
    block_factor = 2.0 ** jax.random.uniform(key_b, (TOKEN_TOTAL // TOK_DEV, 1), jnp.float32, -1.0, 1.0)
    per_token = jnp.repeat(block_factor, TOK_DEV, axis=0)
    data_factor = jnp.exp(jax.random.uniform(key_c, (TOKEN_TOTAL, HEAD_TOTAL), jnp.float32, -1.0, 1.0))
    logarithm_decay_terms = -rate[None, :] * per_token * data_factor
    cluster_positions = jax.random.randint(random_key_fourth, (3,), 0, TOKEN_TOTAL)
    cluster_length = jnp.log(jax.random.uniform(random_key_fifth, (3, HEAD_TOTAL), jnp.float32, 0.5, 0.8))
    cluster_token_count = (jnp.arange(TOKEN_TOTAL, dtype=jnp.int32)[:, None] == cluster_positions[None, :]).astype(jnp.float32)
    token_clusters = jnp.sum(cluster_token_count[:, :, None] * cluster_length[None, :, :], axis=1)
    logarithm_decay_terms = logarithm_decay_terms + jnp.where(slower_decay_heads[None, :], token_clusters, 0.0)
    return jnp.cumsum(logarithm_decay_terms, axis=0)


def draw_residual(key, part):
    key_a = jax.random.fold_in(jax.random.fold_in(key, 31), 0)
    key_c = jax.random.fold_in(jax.random.fold_in(key, 31), 2)
    column = jnp.arange(D, dtype=jnp.float32) / D
    base_draw = jax.random.normal(key_a, (TOKEN_TOTAL, D), jnp.float32)
    col_scale = 0.4 * 5.0 ** column * jax.random.uniform(key_c, (D,), jnp.float32, 0.7, 1.3)
    values = col_scale[None, :] * base_draw
    return jnp.clip(values, -24.0, 24.0).astype(jnp.bfloat16)


def block_scale(key, extent, shards, least, top_value):
    loudness = 1.0
    for axis_at, parts in shards:
        draws = jax.random.uniform(jax.random.fold_in(jax.random.fold_in(key, 6), axis_at), (parts,), jnp.float32, least / len(shards), top_value / len(shards))
        loudness = loudness * jnp.repeat(jnp.exp(draws), extent[axis_at] // parts).reshape((-1,) + (1,) * (len(extent) - 1 - axis_at))
    return loudness


def deal_out(stream_key, own, number, rows, amount, top, bound, lean):
    ranking = jax.random.permutation(stream_key, amount)
    packed, common = portions_of(amount, rows * top, bound, lean, True), portions_of(amount, rows * top, bound, lean, False)
    places = jnp.arange(amount)

    def named(lengths, rotation):
        used = int((lengths > 0).sum())
        fixed = max(1, used // 4)
        shifted = fixed + (places - fixed + rotation * (used - fixed)) % max(1, amount - fixed)
        return jnp.zeros((amount,), jnp.int32).at[ranking[jnp.where(places < fixed, places, shifted)]].set(jnp.asarray(lengths, jnp.int32))

    lengths = jnp.where(number % 4 == 0, named(packed, number // 4), named(common, number - number // 4 - 1))
    mixed = jax.random.permutation(jax.random.fold_in(own, 3), amount)
    donor, sink = mixed[0:amount // 2 * 2:2], mixed[1:amount // 2 * 2:2]
    slack = jnp.minimum(lengths[donor] - 1, bound - lengths[sink]) // 2
    slack = jnp.where((donor == ranking[0]) | (sink == ranking[0]) | (lengths[sink] == 0), 0, jnp.maximum(slack, 0))
    shifted = jax.random.randint(jax.random.fold_in(own, 4), (amount // 2,), 0, 1 << 20) % (slack + 1)
    lengths = lengths.at[donor].add(-shifted).at[sink].add(shifted)
    members = jnp.searchsorted(jnp.cumsum(lengths), jnp.arange(rows * top), side="right").astype(jnp.int32)
    grid = members.reshape(top, rows).T
    grid = grid[jax.random.permutation(jax.random.fold_in(own, 1), rows)]
    rotation = jax.random.randint(jax.random.fold_in(own, 2), (rows, 1), 0, top)
    return jnp.take_along_axis(grid, (jnp.arange(top)[None, :] + rotation) % top, axis=1)


def portions_of(count, total, limit, lean, full):
    loads = [(1 << 20) // math.isqrt(grade ** lean) + 1 for grade in range(1, count + 1)]
    largest = limit if full else min(limit, max(-(-total // count), total * loads[0] // sum(loads)))
    least = 1 if total - largest >= count - 1 else 0
    counts, rest = [largest] + [least] * (count - 1), total - largest - least * (count - 1)
    while rest > 0:
        free = [i for i in range(1, count) if counts[i] < largest] or [i for i in range(1, count) if counts[i] < limit]
        mass, budget = sum([loads[i] for i in free]), rest
        for i in free:
            extra = min(limit - counts[i], max(1, budget * loads[i] // mass), rest)
            counts[i] = counts[i] + extra
            rest = rest - extra
    return np.array(counts)


def normal_values(rng, extent, deviation, bound, pieces=(), kind=jnp.bfloat16):
    loudness = block_scale(rng, extent, pieces, -0.22, 0.18) if pieces else 1.0
    entries = jax.random.normal(rng, extent, jnp.float32) * deviation * loudness
    return jnp.minimum(jnp.maximum(entries, -bound), bound).astype(kind)


def setup_inputs(seed: int = 0) -> dict:
    keys = jax.random.split(jax.random.key(seed), 16)
    queries = draw_queries(jax.random.fold_in(keys[15], 71), 0)
    key_vectors = draw_key_vectors(jax.random.fold_in(keys[15], 71), 0)
    value_vectors = normal_values(keys[2], (TOKEN_TOTAL, HEAD_TOTAL * HDIM), 1.0, 6.0, ((0, 8), (1, 4)))
    log_gate_sums = draw_log_gate_sums(jax.random.fold_in(keys[15], 71), 0)
    residual = draw_residual(jax.random.fold_in(keys[15], 71), 0)
    out_weight = normal_values(keys[5], (HEAD_TOTAL * HDIM, D), (HEAD_TOTAL * HDIM // 16) ** -0.5, 0.75, ((1, 4),))
    norm_gain = jnp.clip(1.0 + 0.18 * jax.random.normal(keys[6], (D,), jnp.float32), 0.099609375, 1.8984375).astype(jnp.bfloat16)
    routes_keys = jax.random.split(jax.random.fold_in(keys[7], 1), TOKEN_TOTAL // TOK_DEV)
    routes_turns = jax.random.permutation(jax.random.fold_in(keys[7], 3), TOKEN_TOTAL // TOK_DEV)
    routes = jax.vmap(lambda own, number: deal_out(jax.random.fold_in(keys[7], 2), own, number, TOK_DEV, EXPERTS, TOPK, CAP, 1))(routes_keys, routes_turns).reshape((TOKEN_TOTAL, TOPK))
    route_weight = jnp.clip(0.5 + 1.0 * jax.random.uniform(keys[8], (TOKEN_TOTAL, TOPK), jnp.float32) ** block_scale(keys[8], (TOKEN_TOTAL, TOPK), ((0, 8),), -0.2, 0.2), 0.5, 1.5)
    expert_gate = normal_values(keys[9], (EXPERTS, D, EF), D ** -0.5, 0.125, ((0, 8), (2, 4)))
    expert_up = normal_values(keys[10], (EXPERTS, D, EF), D ** -0.5, 0.125, ((0, 8), (2, 4)))
    expert_down = normal_values(keys[11], (EXPERTS, EF, D), EF ** -0.5, 0.25, ((0, 8), (2, 4)))
    shared_gate = normal_values(keys[12], (D, SH), D ** -0.5, 0.125, ((1, 4),))
    shared_up = normal_values(keys[13], (D, SH), D ** -0.5, 0.125, ((1, 4),))
    shared_down = normal_values(keys[14], (SH, D), SH ** -0.5, 0.25, ((1, 4),))
    return dict(queries=queries, key_vectors=key_vectors, value_vectors=value_vectors, log_gate_sums=log_gate_sums, residual=residual, out_weight=out_weight, norm_gain=norm_gain, routes=routes, route_weight=route_weight, expert_gate=expert_gate, expert_up=expert_up, expert_down=expert_down, shared_gate=shared_gate, shared_up=shared_up, shared_down=shared_down)


EPSILON = 1e-06

def silu_gate(gate_part, up_part):
    return jax.nn.silu(gate_part) * up_part

def one_head(inputs):
    query_head, key_head, value_head, gate_head = inputs
    block_size = math.gcd(TOKEN_TOTAL, 512)
    key_pos = jnp.arange(TOKEN_TOTAL, dtype=jnp.int32)
    score_scale = HDIM ** (-0.5)

    def one_block(block_number):
        first_row = (block_number * block_size).astype(jnp.int32)
        query_block = lax.dynamic_slice_in_dim(query_head, first_row, block_size, 0)
        gate_block = lax.dynamic_slice_in_dim(gate_head, first_row, block_size, 0)
        scores = jnp.dot(query_block, key_head.T, preferred_element_type=jnp.float32) * score_scale
        scores = scores + gate_block[:, None] - gate_head[None, :]
        query_pos = first_row + jnp.arange(block_size, dtype=jnp.int32)
        allowed = key_pos[None, :] <= query_pos[:, None]
        highest = lax.optimization_barrier(jnp.max(jnp.where(allowed, scores, -jnp.inf), axis=1, keepdims=True))
        weight = jnp.where(allowed, jnp.exp(scores - highest), 0.0)
        weight_total = lax.optimization_barrier(jnp.sum(weight, axis=1, keepdims=True))
        mixed_rows = jnp.dot(weight.astype(jnp.bfloat16), value_head, preferred_element_type=jnp.float32)
        return (mixed_rows / weight_total).astype(jnp.bfloat16)
    blocks_out = lax.map(one_block, jnp.arange(TOKEN_TOTAL // block_size, dtype=jnp.int32))
    return blocks_out.reshape(TOKEN_TOTAL, HDIM)

def block_targets(block_routes):
    flat_routes = block_routes.reshape(-1)
    onehot = (flat_routes[:, None] == jnp.arange(EXPERTS, dtype=jnp.int32)[None, :]).astype(jnp.int32)
    before = jnp.cumsum(onehot, axis=0) - onehot
    return flat_routes * CAP + lax.optimization_barrier(jnp.sum(before * onehot, axis=1))

def reference(queries, key_vectors, value_vectors, log_gate_sums, residual, out_weight, norm_gain, routes, route_weight, expert_gate, expert_up, expert_down, shared_gate, shared_up, shared_down):

    def by_head(matrix):
        return matrix.reshape(TOKEN_TOTAL, HEAD_TOTAL, HDIM).transpose(1, 0, 2)
    attended = lax.map(one_head, (by_head(queries), by_head(key_vectors), by_head(value_vectors), log_gate_sums.T))
    attended = attended.transpose(1, 0, 2).reshape(TOKEN_TOTAL, HEAD_TOTAL * HDIM)
    projected = jnp.dot(attended, out_weight, preferred_element_type=jnp.float32)
    mid = (residual.astype(jnp.float32) + projected).astype(jnp.bfloat16)
    mid_wide = mid.astype(jnp.float32)
    inverse = lax.rsqrt(lax.optimization_barrier(jnp.mean(mid_wide * mid_wide, axis=1, keepdims=True)) + EPSILON)
    normed = (mid_wide * inverse * norm_gain.astype(jnp.float32)).astype(jnp.bfloat16)
    shared_mid = silu_gate(jnp.dot(normed, shared_gate, preferred_element_type=jnp.float32), jnp.dot(normed, shared_up, preferred_element_type=jnp.float32)).astype(jnp.bfloat16)
    shared_out = jnp.dot(shared_mid, shared_down, preferred_element_type=jnp.float32)
    targets = jax.vmap(block_targets)(routes.reshape(N_SP, TOK_DEV, TOPK))
    local_rows = jnp.arange(TOK_DEV * TOPK, dtype=jnp.int32) // TOPK

    def block_owners(target_row, block_number):
        table = jnp.full((EXPERTS * CAP,), TOKEN_TOTAL, jnp.int32)
        return table.at[target_row].set(block_number * TOK_DEV + local_rows)
    owners = jax.vmap(block_owners)(targets, jnp.arange(N_SP, dtype=jnp.int32))
    owners = owners.reshape(N_SP, EXPERTS, CAP).transpose(1, 0, 2).reshape(EXPERTS, N_SP * CAP)
    padded = jnp.concatenate([normed, jnp.zeros((1, D), jnp.bfloat16)], axis=0)

    def one_expert(inputs):
        gate_weight, up_weight, down_weight, owner_rows = inputs
        row_values = padded[owner_rows]
        hidden = silu_gate(jnp.dot(row_values, gate_weight, preferred_element_type=jnp.float32), jnp.dot(row_values, up_weight, preferred_element_type=jnp.float32)).astype(jnp.bfloat16)
        return jnp.dot(hidden, down_weight, preferred_element_type=jnp.float32).astype(jnp.bfloat16)
    produced = lax.map(one_expert, (expert_gate, expert_up, expert_down, owners))
    expert_ids = targets // CAP
    slot_rank = targets % CAP
    block_ids = jnp.arange(N_SP, dtype=jnp.int32)[:, None]
    flat_index = (expert_ids * (N_SP * CAP) + block_ids * CAP + slot_rank).reshape(-1)
    picked = produced.reshape(EXPERTS * N_SP * CAP, D)[flat_index].astype(jnp.float32).reshape(TOKEN_TOTAL, TOPK, D)
    routed = lax.optimization_barrier(jnp.sum(picked * route_weight[:, :, None], axis=1))
    return (mid_wide + shared_out + routed).astype(jnp.bfloat16)
```

```python
import functools
import math

import jax
import jax.numpy as jnp
from jax import lax
from jax.experimental import pallas as pl
from jax.experimental.pallas import tpu as pltpu
from jax.sharding import PartitionSpec as P

HDIM = 64
EPSILON = 1e-06
LOG2E = math.log2(math.e)
LOW = -1e30
F32 = jnp.float32
BF16 = jnp.bfloat16


def silu_gate(gate_part, up_part):
    return jax.nn.silu(gate_part) * up_part


def call(kernel, name, out_shape, args, smem=0, scratch=()):
    vm = pl.BlockSpec(memory_space=pltpu.VMEM)
    sm = pl.BlockSpec(memory_space=pltpu.SMEM)
    single = not isinstance(out_shape, (list, tuple))
    return pl.pallas_call(
        kernel,
        name=name,
        out_shape=out_shape,
        in_specs=[sm] * smem + [vm] * (len(args) - smem),
        out_specs=vm if single else [vm] * len(out_shape),
        scratch_shapes=list(scratch),
    )(*args)


def low_lanes(shape):
    return lax.broadcasted_iota(jnp.int32, shape, 1) < HDIM


def swap_halves(x):
    return pltpu.roll(x, HDIM, 1)


def pack_kernel(heads, q_ref, k_ref, v_ref, g_ref, o_ref):
    tok = q_ref.shape[0]
    half = tok // 2
    low = low_lanes((tok, 2 * HDIM))
    low_half = low_lanes((half, 2 * HDIM))
    gates = g_ref[...].T
    for pair in range(heads // 2):
        cols = slice(pair * 2 * HDIM, (pair + 1) * 2 * HDIM)
        q = q_ref[:, cols].astype(F32)
        k = k_ref[:, cols].astype(F32)
        v = v_ref[:, cols].astype(F32)
        o_ref[2 * pair, 0:tok] = jnp.where(low, k, swap_halves(v)).astype(BF16)
        o_ref[2 * pair + 1, 0:tok] = jnp.where(low, swap_halves(k), v).astype(BF16)
        qa, qb = q[:half], q[half:]
        o_ref[2 * pair, tok : tok + half] = jnp.where(low_half, qa, swap_halves(qb)).astype(BF16)
        o_ref[2 * pair + 1, tok : tok + half] = jnp.where(low_half, swap_halves(qa), qb).astype(BF16)
    rows = tok // 128
    for h in range(heads):
        left = gates[h : h + 1]
        pieces = []
        for _ in range(3):
            piece = left.astype(BF16).astype(F32)
            left = left - piece
            pieces += [piece[:, r * 128 : (r + 1) * 128] for r in range(rows)]
        pad = o_ref.shape[1] - tok - half - len(pieces)
        pieces.append(jnp.zeros((pad, 128), F32))
        o_ref[h, tok + half :] = jnp.concatenate(pieces, axis=0).astype(BF16)


def attn_kernel(nz, tok, c_ref, own_ref, sw_ref, o_ref, kv_scr, vo_scr, g_scr):
    core = c_ref[0]
    half = tok // 2
    wide = 2 * tok
    rows = tok // 128
    low_tok = low_lanes((tok, 128))
    low_half = low_lanes((half, 128))
    for z in range(nz):
        for ref, at in ((own_ref, core), (sw_ref, 1 - core)):
            kv = ref[z, 0:tok]
            spot = pl.ds(pl.multiple_of(at * tok, tok), tok)
            kv_scr[z, spot] = kv
            vo_scr[z, spot] = jnp.where(low_tok, 1.0, kv.astype(F32)).astype(BF16)
            g = ref[z, tok + half :].astype(F32)
            g = (g[0:rows] + g[rows : 2 * rows] + g[2 * rows : 3 * rows]) * LOG2E
            g = jnp.concatenate([g[r : r + 1] for r in range(rows)], axis=1)
            g_scr[z, 0:1, spot] = g
    scale = HDIM ** (-0.5) * LOG2E

    def step(q, z, state, mask=None):
        m, acc = state
        s = lax.dot_general(q, kv_scr[z], (((1,), (1,)), ((), ())), preferred_element_type=F32)
        t = s * scale - g_scr[z, 0:1]
        if mask is not None:
            t = jnp.where(mask, t, LOW)
        top = jnp.maximum(m, jnp.max(t, axis=1, keepdims=True))
        p = jnp.exp2(t - top)
        acc = acc * jnp.exp2(m - top) + jnp.dot(p.astype(BF16), vo_scr[z], preferred_element_type=F32)
        return top, acc

    key_at = lax.broadcasted_iota(jnp.int32, (half, wide), 1)
    row_at = lax.broadcasted_iota(jnp.int32, (half, wide), 0) + core * tok

    def one_block(zq, carry):
        packed = own_ref[zq, tok : tok + half].astype(F32)
        qs = (
            jnp.where(low_half, packed, 0.0).astype(BF16),
            jnp.where(low_half, swap_halves(packed), 0.0).astype(BF16),
        )
        start = tuple((jnp.full((half, 1), LOW, F32), jnp.zeros((half, 128), F32)) for _ in qs)
        state = lax.fori_loop(0, zq, lambda z, st: tuple(step(q, z, s) for q, s in zip(qs, st)), start)
        state = tuple(
            step(q, zq, s, key_at <= row_at + i * half) for i, (q, s) in enumerate(zip(qs, state))
        )
        acc_a, acc_b = state[0][1], state[1][1]
        out_a = swap_halves(acc_a) / acc_a
        out_b = acc_b / swap_halves(acc_b)
        o_ref[zq] = jnp.where(low_half, out_a, out_b).astype(BF16)
        return carry

    lax.fori_loop(0, nz, one_block, 0)


def route_kernel(experts, cap, rt_ref, rc_ref, d_ref, c0_ref, c1_ref):
    tok = rc_ref.shape[0]
    slots = experts * cap
    at = lax.broadcasted_iota(jnp.int32, (tok, tok), 0)
    bt = lax.broadcasted_iota(jnp.int32, (tok, tok), 1)
    eid = lax.broadcasted_iota(jnp.int32, (experts, tok), 0)
    hot = [jnp.where(eid == rt_ref[k : k + 1], 1.0, 0.0) for k in range(2)]
    before = jnp.where(at < bt, 1.0, 0.0).astype(BF16)
    rank = jnp.dot((hot[0] + hot[1]).astype(BF16), before, preferred_element_type=F32)
    place = rank + (eid * cap).astype(F32)
    rows = [jnp.sum(h * place, axis=0, keepdims=True).astype(jnp.int32) for h in hot]
    sid = lax.broadcasted_iota(jnp.int32, (slots, tok), 0)
    d_ref[...] = jnp.where((sid == rows[0]) | (sid == rows[1]), 1.0, 0.0).astype(BF16)
    eid = lax.broadcasted_iota(jnp.int32, (tok, experts), 1)
    hot = [jnp.where(eid == rc_ref[:, k : k + 1], 1.0, 0.0) for k in range(2)]
    after = jnp.where(bt < at, 1.0, 0.0).astype(BF16)
    rank = jnp.dot(after, (hot[0] + hot[1]).astype(BF16), preferred_element_type=F32)
    place = rank + (eid * cap).astype(F32)
    cols = [jnp.sum(h * place, axis=1, keepdims=True).astype(jnp.int32) for h in hot]
    sid = lax.broadcasted_iota(jnp.int32, (tok, slots), 1)
    c0_ref[...] = jnp.where(sid == cols[0], 1.0, 0.0).astype(BF16)
    c1_ref[...] = jnp.where(sid == cols[1], 1.0, 0.0).astype(BF16)


def mid_kernel(heads, cap, t_ref, *refs):
    n = len(refs) - 5
    parts, (w_ref, r_ref, d_ref, m_ref, out_ref) = refs[:n], refs[n:]
    half = parts[0].shape[1]
    width = heads * HDIM
    low = low_lanes((half, 2 * HDIM))
    tops = [None, None]
    for k in range(n):
        src = t_ref[0] ^ k
        w = w_ref[pl.ds(pl.multiple_of(src * width, width), width), :]
        ab = ([], [])
        for pair in range(heads // 2):
            p0 = parts[k][2 * pair].astype(F32)
            p1 = parts[k][2 * pair + 1].astype(F32)
            ab[0].append(jnp.where(low, p0, swap_halves(p1)).astype(BF16))
            ab[1].append(jnp.where(low, swap_halves(p0), p1).astype(BF16))
        for i in range(2):
            got = jnp.dot(jnp.concatenate(ab[i], axis=1), w, preferred_element_type=F32)
            tops[i] = got if tops[i] is None else tops[i] + got
    for i in range(2):
        rows = slice(i * half, (i + 1) * half)
        m_ref[rows] = (r_ref[rows].astype(F32) + tops[i]).astype(BF16)
    mid = m_ref[...]
    experts = out_ref.shape[0]
    group = 4
    for e in range(0, experts, group):
        got = jnp.dot(d_ref[e * cap : (e + group) * cap], mid, preferred_element_type=F32)
        for i in range(group):
            out_ref[e + i] = got[i * cap : (i + 1) * cap].astype(BF16)


def normed_of(parts, gains, width):
    total = None
    for x in parts:
        sq = jnp.sum(x * x, axis=1, keepdims=True)
        total = sq if total is None else total + sq
    inverse = lax.rsqrt(total / width + EPSILON)
    return [(x * inverse * g).astype(BF16) for x, g in zip(parts, gains)]


def shared_kernel(t_ref, *refs):
    n = len(refs) - 4
    parts, (gain_ref, gate_ref, up_ref, o_ref) = refs[:n], refs[n:]
    part_width = parts[0].shape[1]
    width = n * part_width
    srcs = [t_ref[0] ^ k for k in range(n)]
    normed = normed_of([p[...].astype(F32) for p in parts], [gain_ref[s] for s in srcs], width)
    both = None
    for s, x in zip(srcs, normed):
        rows = pl.ds(pl.multiple_of(s * part_width, part_width), part_width)
        w = jnp.concatenate([gate_ref[rows, :], up_ref[rows, :]], axis=1)
        got = jnp.dot(x, w, preferred_element_type=F32)
        both = got if both is None else both + got
    hid = gate_ref.shape[1]
    o_ref[...] = silu_gate(both[:, :hid], both[:, hid:]).astype(BF16)


def expert_kernel(sp, tp, t_ref, x_ref, gain_ref, *refs):
    gates, ups, downs = refs[:tp], refs[tp : 2 * tp], refs[2 * tp : 3 * tp]
    y_ref, x_scr, h_scr = refs[3 * tp :]
    me = t_ref[0]
    cap, part_width = x_ref.shape[1:]
    parts = [
        jnp.concatenate([x_ref[s * tp + t].astype(F32) for s in range(sp)], axis=0) for t in range(tp)
    ]
    normed = normed_of(parts, [gain_ref[t] for t in range(tp)], tp * part_width)
    for t in range(tp):
        x_scr[:, t * part_width : (t + 1) * part_width] = normed[t]
    x = x_scr[...]
    hid = gates[0].shape[1]
    for k in range(tp):
        w = jnp.concatenate([gates[k][...], ups[k][...]], axis=1)
        both = jnp.dot(x, w, preferred_element_type=F32)
        spot = pl.ds(pl.multiple_of((me ^ k) * hid, hid), hid)
        h_scr[:, spot] = silu_gate(both[:, :hid], both[:, hid:]).astype(BF16)
    h = h_scr[...]
    for k in range(tp):
        y = jnp.dot(h, downs[k][...], preferred_element_type=F32)
        for s in range(sp):
            y_ref[s * tp + (me ^ k)] = y[s * cap : (s + 1) * cap].astype(BF16)


def final_kernel(t_ref, *refs):
    n = len(refs) - 8
    hids = refs[:n]
    down_ref, mid_ref, ret_ref, c0_ref, c1_ref, w_ref, o_ref, h_scr = refs[n:]
    hid = hids[0].shape[1]
    for k in range(n):
        spot = pl.ds(pl.multiple_of((t_ref[0] ^ k) * hid, hid), hid)
        h_scr[:, spot] = hids[k][...]
    out = jnp.dot(h_scr[...], down_ref[...], preferred_element_type=F32)
    experts, cap, width = ret_ref.shape
    rows = ret_ref[...].astype(F32).reshape(experts * cap, width).astype(BF16)
    out = out + mid_ref[...].astype(F32)
    out = out + w_ref[:, 0:1] * jnp.dot(c0_ref[...], rows, preferred_element_type=F32)
    out = out + w_ref[:, 1:2] * jnp.dot(c1_ref[...], rows, preferred_element_type=F32)
    o_ref[...] = out.astype(BF16)


def shards(
    queries,
    key_vectors,
    value_vectors,
    log_gate_sums,
    residual,
    out_weight,
    norm_gain,
    routes,
    route_weight,
    expert_gate,
    expert_up,
    expert_down,
    shared_gate,
    shared_up,
    shared_down,
):
    sp, tp = lax.axis_size("sp"), lax.axis_size("tp")
    tok = queries.shape[0]
    heads = log_gate_sums.shape[1]
    width = residual.shape[1]
    exp_dev = expert_gate.shape[0]
    experts = exp_dev * sp
    top_count = routes.shape[1]
    cap = 5 * tok * top_count // (4 * experts)
    nz = sp // 2
    me = lax.axis_index("tp")
    me_ref = me.astype(jnp.int32).reshape(1)
    core_ref = (lax.axis_index("sp") % 2).astype(jnp.int32).reshape(1)
    half = tok // 2
    rows = tok + half + -(-3 * (tok // 128) // 16) * 16

    def over_tp(x, k):
        return lax.ppermute(x, "tp", [(i, i ^ k) for i in range(tp)])

    def all_tp(x):
        return [x] + [over_tp(x, k) for k in range(1, tp)]

    slab = call(
        functools.partial(pack_kernel, heads),
        "pack",
        jax.ShapeDtypeStruct((heads, rows, 128), BF16),
        (queries, key_vectors, value_vectors, log_gate_sums),
    )
    groups = [[2 * z + c for z in range(nz)] for c in range(2)]
    own = lax.all_to_all(slab, "sp", 0, 0, tiled=True, axis_index_groups=groups)
    swapped = lax.ppermute(own, "sp", [(i, i ^ 1) for i in range(sp)])
    mixed = call(
        functools.partial(attn_kernel, nz, tok),
        "attention",
        jax.ShapeDtypeStruct((nz, half, 128), BF16),
        (core_ref, own, swapped),
        smem=1,
        scratch=(
            pltpu.VMEM((nz, 2 * tok, 128), BF16),
            pltpu.VMEM((nz, 2 * tok, 128), BF16),
            pltpu.VMEM((nz, 8, 2 * tok), F32),
        ),
    )
    attended = lax.all_to_all(mixed, "sp", 0, 0, tiled=True, axis_index_groups=groups)

    def deal(weights):
        pieces = [lax.dynamic_index_in_dim(weights, me ^ k, 0, keepdims=False) for k in range(tp)]
        return pieces[:1] + [over_tp(pieces[k], k) for k in range(1, tp)]

    gates, ups, downs = deal(expert_gate), deal(expert_up), deal(expert_down)

    spread, pick0, pick1 = call(
        functools.partial(route_kernel, experts, cap),
        "route",
        [
            jax.ShapeDtypeStruct((experts * cap, tok), BF16),
            jax.ShapeDtypeStruct((tok, experts * cap), BF16),
            jax.ShapeDtypeStruct((tok, experts * cap), BF16),
        ],
        (routes.T, routes),
    )
    gain = norm_gain.astype(F32).reshape(tp, 1, width)

    mid, outgoing = call(
        functools.partial(mid_kernel, heads, cap),
        "mid",
        [
            jax.ShapeDtypeStruct((tok, width), BF16),
            jax.ShapeDtypeStruct((experts, cap, width), BF16),
        ],
        (me_ref, *all_tp(attended), out_weight, residual, spread),
        smem=1,
    )
    mids = all_tp(mid)
    arrived = lax.all_to_all(outgoing, ("sp", "tp"), 0, 0, tiled=True)
    shared_mid = call(
        shared_kernel,
        "shared",
        jax.ShapeDtypeStruct((tok, shared_gate.shape[1]), BF16),
        (me_ref, *mids, gain, shared_gate, shared_up),
        smem=1,
    )
    shared_mids = all_tp(shared_mid)
    produced = call(
        functools.partial(expert_kernel, sp, tp),
        "expert",
        jax.ShapeDtypeStruct((sp * tp, cap, width), BF16),
        (me_ref, arrived, gain, *gates, *ups, *downs),
        smem=1,
        scratch=(
            pltpu.VMEM((sp * cap, tp * width), BF16),
            pltpu.VMEM((sp * cap, tp * expert_gate.shape[2]), BF16),
        ),
    )
    returned = lax.all_to_all(produced, ("sp", "tp"), 0, 0, tiled=True)
    return call(
        final_kernel,
        "final",
        jax.ShapeDtypeStruct((tok, width), BF16),
        (me_ref, *shared_mids, shared_down, mid, returned, pick0, pick1, route_weight),
        smem=1,
        scratch=(pltpu.VMEM((tok, shared_down.shape[0]), BF16),),
    )


def slot_targets(routes, experts_all, capacity):
    flat_routes = routes.reshape(-1)
    onehot = (flat_routes[:, None] == jnp.arange(experts_all, dtype=jnp.int32)[None, :]).astype(
        jnp.int32
    )
    before = jnp.cumsum(onehot, axis=0) - onehot
    return flat_routes * capacity + jnp.sum(before * onehot, axis=1)


def keep_state(fold_state):
    return fold_state


def generic_shards(
    queries,
    key_vectors,
    value_vectors,
    log_gate_sums,
    residual,
    out_weight,
    norm_gain,
    routes,
    route_weight,
    expert_gate,
    expert_up,
    expert_down,
    shared_gate,
    shared_up,
    shared_down,
):
    tok_dev = queries.shape[0]
    head_dim = HDIM
    local_heads = log_gate_sums.shape[1]
    local_width = residual.shape[1]
    model_width = norm_gain.shape[0]
    score_scale = head_dim ** (-0.5)
    seq_first = lax.axis_index("sp") * tok_dev
    query_heads = queries.reshape(tok_dev, local_heads, head_dim)
    query_pos = seq_first + jnp.arange(tok_dev, dtype=jnp.int32)
    own_gates = log_gate_sums.T
    all_gates = lax.all_gather(log_gate_sums, "sp", axis=0, tiled=True)
    initial = (
        jnp.full((local_heads, tok_dev), -1e30, jnp.float32),
        jnp.zeros((local_heads, tok_dev), jnp.float32),
        jnp.zeros((local_heads, tok_dev, head_dim), jnp.float32),
    )
    key_heads = key_vectors.reshape(tok_dev, local_heads, head_dim)
    value_heads = value_vectors.reshape(tok_dev, local_heads, head_dim)
    key_part = lax.all_gather(key_heads, "sp", axis=0, tiled=True)
    value_part = lax.all_gather(value_heads, "sp", axis=0, tiled=True)
    part_rows = key_part.shape[0]
    block_size = math.gcd(part_rows, 512)
    key_blocks = key_part.reshape(part_rows // block_size, block_size, local_heads, head_dim)
    value_blocks = value_part.reshape(part_rows // block_size, block_size, local_heads, head_dim)

    def one_block(fold_state, inputs):
        key_block, value_block, block_number = inputs
        block_first = block_number * block_size

        def compute(old_state):
            running_max, weight_total, summed = old_state
            gate_block = lax.dynamic_slice_in_dim(all_gates, block_first, block_size, 0).T
            scores = (
                jnp.einsum(
                    "qhd,khd->hqk", query_heads, key_block, preferred_element_type=jnp.float32
                )
                * score_scale
            )
            scores = scores + own_gates[:, :, None] - gate_block[:, None, :]
            key_pos = block_first + jnp.arange(block_size, dtype=jnp.int32)
            allowed = (key_pos[None, :] <= query_pos[:, None])[None]
            newmax = jnp.maximum(running_max, jnp.max(jnp.where(allowed, scores, -jnp.inf), axis=2))
            factor = jnp.exp(running_max - newmax)
            weight = jnp.where(allowed, jnp.exp(scores - newmax[:, :, None]), 0.0)
            weight_total = weight_total * factor + jnp.sum(weight, axis=2)
            summed = summed * factor[:, :, None] + jnp.einsum(
                "hqk,khd->hqd",
                weight.astype(jnp.bfloat16),
                value_block,
                preferred_element_type=jnp.float32,
            )
            return (newmax, weight_total, summed)

        useful = block_first <= seq_first + tok_dev - 1
        return (lax.cond(useful, compute, keep_state, fold_state), None)

    numbers = jnp.arange(part_rows // block_size, dtype=jnp.int32)
    result_state, _ = lax.scan(one_block, initial, (key_blocks, value_blocks, numbers))
    running_max, weight_total, summed = result_state
    attended = (summed / weight_total[:, :, None]).astype(jnp.bfloat16)
    attended = attended.transpose(1, 0, 2).reshape(tok_dev, local_heads * head_dim)
    weight_rows = out_weight
    projected = jnp.dot(
        lax.all_gather(attended, "tp", axis=1, tiled=True),
        weight_rows,
        preferred_element_type=jnp.float32,
    )
    mid = (residual.astype(jnp.float32) + projected).astype(jnp.bfloat16)
    mid_wide = mid.astype(jnp.float32)
    feature_first = lax.axis_index("tp") * local_width
    squares = lax.psum(jnp.sum(mid_wide * mid_wide, axis=1), "tp")
    inverse = lax.rsqrt(squares / model_width + EPSILON)
    own_gain = lax.dynamic_slice_in_dim(norm_gain, feature_first, local_width, 0).astype(
        jnp.float32
    )
    normed_own = (mid_wide * inverse[:, None] * own_gain[None, :]).astype(jnp.bfloat16)
    normed = lax.all_gather(normed_own, "tp", axis=1, tiled=True)
    shared_mid = silu_gate(
        jnp.dot(normed, shared_gate, preferred_element_type=jnp.float32),
        jnp.dot(normed, shared_up, preferred_element_type=jnp.float32),
    ).astype(jnp.bfloat16)
    weight_rows = shared_down
    shared_out = jnp.dot(
        lax.all_gather(shared_mid, "tp", axis=1, tiled=True),
        weight_rows,
        preferred_element_type=jnp.float32,
    )
    exp_dev = expert_gate.shape[0]
    sp_count = lax.axis_size("sp")
    experts_all = exp_dev * sp_count
    top_count = routes.shape[1]
    capacity = 5 * tok_dev * top_count // (4 * experts_all)
    targets = slot_targets(routes, experts_all, capacity)
    owners = (
        jnp.full((experts_all * capacity,), tok_dev, jnp.int32)
        .at[targets]
        .set(jnp.arange(tok_dev * top_count, dtype=jnp.int32) // top_count)
    )
    padded = jnp.concatenate(
        [normed_own, jnp.zeros((1, normed_own.shape[1]), jnp.bfloat16)], axis=0
    )
    outgoing = padded[owners].reshape(sp_count, exp_dev, capacity, normed_own.shape[1])
    rows_all = lax.all_gather(
        lax.all_to_all(outgoing, "sp", split_axis=0, concat_axis=0, tiled=True),
        "tp",
        axis=3,
        tiled=True,
    )
    gate_part = jnp.einsum(
        "secd,edf->secf", rows_all, expert_gate, preferred_element_type=jnp.float32
    )
    up_part = jnp.einsum("secd,edf->secf", rows_all, expert_up, preferred_element_type=jnp.float32)
    hidden = silu_gate(gate_part, up_part).astype(jnp.bfloat16)
    hidden_all = lax.all_gather(hidden, "tp", axis=3, tiled=True)
    produced = jnp.einsum(
        "secf,efd->secd", hidden_all, expert_down, preferred_element_type=jnp.float32
    ).astype(jnp.bfloat16)
    returned = lax.all_to_all(produced, "sp", split_axis=0, concat_axis=0, tiled=True)
    returned_flat = returned.reshape(experts_all * capacity, local_width)
    picked = returned_flat[targets].astype(jnp.float32).reshape(tok_dev, top_count, local_width)
    routed = jnp.sum(picked * route_weight[:, :, None], axis=1)
    return (mid_wide + shared_out + routed).astype(jnp.bfloat16)


def solution(mesh):
    placed = (
        P("sp", "tp"),
        P("sp", "tp"),
        P("sp", "tp"),
        P("sp", "tp"),
        P("sp", "tp"),
        P(None, "tp"),
        P(),
        P("sp", None),
        P("sp", None),
        P("sp", None, "tp"),
        P("sp", None, "tp"),
        P("sp", None, "tp"),
        P(None, "tp"),
        P(None, "tp"),
        P(None, "tp"),
    )
    sp, tp = mesh.shape["sp"], mesh.shape["tp"]

    def program(*args):
        heads = args[3].shape[1] // tp
        exp_dev = args[9].shape[0] // sp
        deals = sp % 2 == 0 and heads * 2 == sp and exp_dev == tp and tp & (tp - 1) == 0
        body = shards if deals else generic_shards
        mapped = jax.shard_map(body, mesh=mesh, in_specs=placed, out_specs=P("sp", "tp"), check_vma=False)
        return mapped(*args)

    return program
```

```python
import functools
import math

import jax
import jax.numpy as jnp
from jax import lax
from jax.experimental import pallas as pl
from jax.experimental.pallas import tpu as pltpu
from jax.sharding import PartitionSpec as P


HDIM = 64
EPSILON = 1e-06
LOG2E = math.log2(math.e)
LOW = -1e30
F32 = jnp.float32
BF16 = jnp.bfloat16


def silu_gate(gate_part, up_part):
    return jax.nn.silu(gate_part) * up_part


def call(kernel, out_shape, args, smem=0, scratch=()):
    vm = pl.BlockSpec(memory_space=pltpu.VMEM)
    sm = pl.BlockSpec(memory_space=pltpu.SMEM)
    single = not isinstance(out_shape, (list, tuple))
    return pl.pallas_call(
        kernel,
        out_shape=out_shape,
        in_specs=[sm] * smem + [vm] * (len(args) - smem),
        out_specs=vm if single else [vm] * len(out_shape),
        scratch_shapes=list(scratch),
    )(*args)


def low_lanes(shape):
    return lax.broadcasted_iota(jnp.int32, shape, 1) < HDIM


def swap_halves(x):
    return pltpu.roll(x, HDIM, 1)


def pack_kernel(heads, z_ref, q_ref, k_ref, v_ref, g_ref, *slabs):
    tok = q_ref.shape[0]
    half = tok // 2
    low = low_lanes((tok, 2 * HDIM))
    low_half = low_lanes((half, 2 * HDIM))
    o_ref = slabs[-1]
    slabs = slabs[:-1]
    gates = g_ref[...]
    for pair in range(heads // 2):
        cols = slice(pair * 2 * HDIM, (pair + 1) * 2 * HDIM)
        q = q_ref[:, cols].astype(F32)
        k = k_ref[:, cols].astype(F32)
        v = v_ref[:, cols].astype(F32)
        o_ref[2 * pair, 0:tok] = jnp.where(low, k, swap_halves(v)).astype(BF16)
        o_ref[2 * pair + 1, 0:tok] = jnp.where(low, swap_halves(k), v).astype(BF16)
        qa, qb = q[:half], q[half:]
        o_ref[2 * pair, tok : tok + half] = jnp.where(low_half, qa, swap_halves(qb)).astype(BF16)
        o_ref[2 * pair + 1, tok : tok + half] = jnp.where(low_half, swap_halves(qa), qb).astype(BF16)
    rows = tok // 128
    for h in range(heads):
        left = gates[h : h + 1]
        pieces = []
        for _ in range(3):
            piece = left.astype(BF16).astype(F32)
            left = left - piece
            pieces += [piece[:, r * 128 : (r + 1) * 128] for r in range(rows)]
        pad = o_ref.shape[1] - tok - half - len(pieces)
        pieces.append(jnp.zeros((pad, 128), F32))
        o_ref[h, tok + half :] = jnp.concatenate(pieces, axis=0).astype(BF16)
    for i, slab in enumerate(slabs):
        slab[...] = o_ref[z_ref[0] ^ i]


def attn_kernel(nz, tok, c_ref, z_ref, *refs):
    owns, sws, outs = refs[:nz], refs[nz : 2 * nz], refs[2 * nz : 3 * nz]
    kv_scr, vo_scr, g_scr, q_scr, o_scr = refs[3 * nz :]
    core = c_ref[0]
    half = tok // 2
    wide = 2 * tok
    rows = tok // 128
    low_tok = low_lanes((tok, 128))
    low_half = low_lanes((half, 128))
    for i in range(nz):
        z = z_ref[0] ^ i
        q_scr[z] = owns[i][tok : tok + half]
        for ref, at in ((owns[i], core), (sws[i], 1 - core)):
            kv = ref[0:tok]
            spot = pl.ds(pl.multiple_of(at * tok, tok), tok)
            kv_scr[z, spot] = kv
            vo_scr[z, spot] = jnp.where(low_tok, 1.0, kv.astype(F32)).astype(BF16)
            g = ref[tok + half :].astype(F32)
            g = (g[0:rows] + g[rows : 2 * rows] + g[2 * rows : 3 * rows]) * LOG2E
            g = jnp.concatenate([g[r : r + 1] for r in range(rows)], axis=1)
            g_scr[z, 0:1, spot] = g
    scale = HDIM ** (-0.5) * LOG2E

    def step(q, z, state, mask=None):
        m, acc = state
        s = lax.dot_general(q, kv_scr[z], (((1,), (1,)), ((), ())), preferred_element_type=F32)
        t = s * scale - g_scr[z, 0:1]
        if mask is not None:
            t = jnp.where(mask, t, LOW)
        top = jnp.maximum(m, jnp.max(t, axis=1, keepdims=True))
        p = jnp.exp2(t - top)
        acc = acc * jnp.exp2(m - top) + jnp.dot(p.astype(BF16), vo_scr[z], preferred_element_type=F32)
        return top, acc

    key_at = lax.broadcasted_iota(jnp.int32, (half, wide), 1)
    row_at = lax.broadcasted_iota(jnp.int32, (half, wide), 0) + core * tok

    def one_block(zq, carry):
        packed = q_scr[zq].astype(F32)
        qs = (
            jnp.where(low_half, packed, 0.0).astype(BF16),
            jnp.where(low_half, swap_halves(packed), 0.0).astype(BF16),
        )
        start = tuple((jnp.full((half, 1), LOW, F32), jnp.zeros((half, 128), F32)) for _ in qs)
        state = lax.fori_loop(0, zq, lambda z, st: tuple(step(q, z, s) for q, s in zip(qs, st)), start)
        state = tuple(
            step(q, zq, s, key_at <= row_at + i * half) for i, (q, s) in enumerate(zip(qs, state))
        )
        acc_a, acc_b = state[0][1], state[1][1]
        out_a = swap_halves(acc_a) / acc_a
        out_b = acc_b / swap_halves(acc_b)
        o_scr[zq] = jnp.where(low_half, out_a, out_b).astype(BF16)
        return carry

    lax.fori_loop(0, nz, one_block, 0)
    for i in range(nz):
        outs[i][...] = o_scr[z_ref[0] ^ i]


def route_kernel(experts, cap, rt_ref, d_ref, c0_ref, c1_ref):
    tok = rt_ref.shape[1]
    slots = experts * cap
    at = lax.broadcasted_iota(jnp.int32, (tok, tok), 0)
    bt = lax.broadcasted_iota(jnp.int32, (tok, tok), 1)
    eid = lax.broadcasted_iota(jnp.int32, (experts, tok), 0)
    hot = [jnp.where(eid == rt_ref[k : k + 1], 1.0, 0.0) for k in range(2)]
    before = jnp.where(at < bt, 1.0, 0.0).astype(BF16)
    rank = jnp.dot((hot[0] + hot[1]).astype(BF16), before, preferred_element_type=F32)
    place = rank + (eid * cap).astype(F32)
    rows = [jnp.sum(h * place, axis=0, keepdims=True).astype(jnp.int32) for h in hot]
    sid = lax.broadcasted_iota(jnp.int32, (slots, tok), 0)
    d_ref[...] = jnp.where((sid == rows[0]) | (sid == rows[1]), 1.0, 0.0).astype(BF16)
    cols = jnp.concatenate([r.astype(F32) for r in rows] * 4, axis=0).T.astype(jnp.int32)
    cols = [cols[:, k : k + 1] for k in range(2)]
    sid = lax.broadcasted_iota(jnp.int32, (tok, slots), 1)
    c0_ref[...] = jnp.where(sid == cols[0], 1.0, 0.0).astype(BF16)
    c1_ref[...] = jnp.where(sid == cols[1], 1.0, 0.0).astype(BF16)


def mid_kernel(heads, cap, t_ref, z_ref, *refs):
    n = len(refs) - 5
    parts, (w_ref, r_ref, d_ref, m_ref, out_ref) = refs[:n], refs[n:]
    half = parts[0].shape[1]
    width = heads * HDIM
    low = low_lanes((half, 2 * HDIM))
    tops = [None, None]
    for k in range(n):
        src = t_ref[0] ^ k
        w = w_ref[pl.ds(pl.multiple_of(src * width, width), width), :]
        ab = ([], [])
        for pair in range(heads // 2):
            p0 = parts[k][z_ref[0] ^ (2 * pair)].astype(F32)
            p1 = parts[k][z_ref[0] ^ (2 * pair + 1)].astype(F32)
            ab[0].append(jnp.where(low, p0, swap_halves(p1)).astype(BF16))
            ab[1].append(jnp.where(low, swap_halves(p0), p1).astype(BF16))
        for i in range(2):
            got = jnp.dot(jnp.concatenate(ab[i], axis=1), w, preferred_element_type=F32)
            tops[i] = got if tops[i] is None else tops[i] + got
    for i in range(2):
        rows = slice(i * half, (i + 1) * half)
        m_ref[rows] = (r_ref[rows].astype(F32) + tops[i]).astype(BF16)
    mid = m_ref[...]
    experts = out_ref.shape[0]
    group = 4
    for e in range(0, experts, group):
        got = jnp.dot(d_ref[e * cap : (e + group) * cap], mid, preferred_element_type=F32)
        for i in range(group):
            out_ref[e + i] = got[i * cap : (i + 1) * cap].astype(BF16)


def normed_of(parts, gains, width):
    total = None
    for x in parts:
        sq = jnp.sum(x * x, axis=1, keepdims=True)
        total = sq if total is None else total + sq
    inverse = lax.rsqrt(total / width + EPSILON)
    return [(x * inverse * g).astype(BF16) for x, g in zip(parts, gains)]


def shared_kernel(t_ref, *refs):
    n = len(refs) - 4
    parts, (gain_ref, gate_ref, up_ref, o_ref) = refs[:n], refs[n:]
    part_width = parts[0].shape[1]
    width = n * part_width
    srcs = [t_ref[0] ^ k for k in range(n)]
    normed = normed_of([p[...].astype(F32) for p in parts], [gain_ref[s] for s in srcs], width)
    both = None
    for s, x in zip(srcs, normed):
        rows = pl.ds(pl.multiple_of(s * part_width, part_width), part_width)
        w = jnp.concatenate([gate_ref[rows, :], up_ref[rows, :]], axis=1)
        got = jnp.dot(x, w, preferred_element_type=F32)
        both = got if both is None else both + got
    hid = gate_ref.shape[1]
    o_ref[...] = silu_gate(both[:, :hid], both[:, hid:]).astype(BF16)


def expert_kernel(sp, tp, t_ref, x_ref, gain_ref, *refs):
    pairs, downs = refs[:tp], refs[tp : 2 * tp]
    y_ref, x_scr, h_scr = refs[2 * tp :]
    me = t_ref[0]
    cap, part_width = x_ref.shape[1:]
    parts = [
        jnp.concatenate([x_ref[s * tp + t].astype(F32) for s in range(sp)], axis=0) for t in range(tp)
    ]
    normed = normed_of(parts, [gain_ref[t] for t in range(tp)], tp * part_width)
    for t in range(tp):
        x_scr[:, t * part_width : (t + 1) * part_width] = normed[t]
    x = x_scr[...]
    hid = pairs[0].shape[1] // 2
    for k in range(tp):
        both = jnp.dot(x, pairs[k][...], preferred_element_type=F32)
        spot = pl.ds(pl.multiple_of((me ^ k) * hid, hid), hid)
        h_scr[:, spot] = silu_gate(both[:, :hid], both[:, hid:]).astype(BF16)
    h = h_scr[...]
    for k in range(tp):
        y = jnp.dot(h, downs[k][...], preferred_element_type=F32)
        for s in range(sp):
            y_ref[s * tp + (me ^ k)] = y[s * cap : (s + 1) * cap].astype(BF16)


def final_kernel(t_ref, *refs):
    n = len(refs) - 8
    hids = refs[:n]
    down_ref, mid_ref, ret_ref, c0_ref, c1_ref, w_ref, o_ref, h_scr = refs[n:]
    hid = hids[0].shape[1]
    for k in range(n):
        spot = pl.ds(pl.multiple_of((t_ref[0] ^ k) * hid, hid), hid)
        h_scr[:, spot] = hids[k][...]
    out = jnp.dot(h_scr[...], down_ref[...], preferred_element_type=F32)
    experts, cap, width = ret_ref.shape
    rows = ret_ref[...].astype(F32).reshape(experts * cap, width).astype(BF16)
    out = out + mid_ref[...].astype(F32)
    w = jnp.concatenate([w_ref[...]] * 4, axis=0).T
    out = out + w[:, 0:1] * jnp.dot(c0_ref[...], rows, preferred_element_type=F32)
    out = out + w[:, 1:2] * jnp.dot(c1_ref[...], rows, preferred_element_type=F32)
    o_ref[...] = out.astype(BF16)


def shards(
    queries,
    key_vectors,
    value_vectors,
    log_gate_sums,
    residual,
    out_weight,
    norm_gain,
    routes,
    route_weight,
    expert_gate,
    expert_up,
    expert_down,
    shared_gate,
    shared_up,
    shared_down,
):
    sp, tp = lax.axis_size("sp"), lax.axis_size("tp")
    tok = queries.shape[0]
    heads = log_gate_sums.shape[1]
    width = residual.shape[1]
    exp_dev = expert_gate.shape[0]
    experts = exp_dev * sp
    top_count = routes.shape[1]
    cap = 5 * tok * top_count // (4 * experts)
    nz = sp // 2
    me = lax.axis_index("tp")
    me_ref = me.astype(jnp.int32).reshape(1)
    core_ref = (lax.axis_index("sp") % 2).astype(jnp.int32).reshape(1)
    half = tok // 2
    rows = tok + half + -(-3 * (tok // 128) // 16) * 16

    def over_tp(x, k):
        return lax.ppermute(x, "tp", [(i, i ^ k) for i in range(tp)])

    def all_tp(x):
        return [x] + [over_tp(x, k) for k in range(1, tp)]

    z = lax.axis_index("sp") // 2
    z_ref = z.astype(jnp.int32).reshape(1)

    def over_z(x, k):
        return lax.ppermute(x, "sp", [(i, i ^ (2 * k)) for i in range(sp)])

    slabs = call(
        functools.partial(pack_kernel, heads),
        [jax.ShapeDtypeStruct((rows, 128), BF16)] * heads,
        (z_ref, queries, key_vectors, value_vectors, log_gate_sums.T),
        smem=1,
        scratch=(pltpu.VMEM((heads, rows, 128), BF16),),
    )
    owns = [slabs[0]] + [over_z(slabs[k], k) for k in range(1, nz)]
    swapped = [lax.ppermute(x, "sp", [(i, i ^ 1) for i in range(sp)]) for x in owns]

    def deal(pieces):
        return pieces[:1] + [over_tp(pieces[k], k) for k in range(1, tp)]

    def pick(weights, k):
        return lax.dynamic_index_in_dim(weights, me ^ k, 0, keepdims=False)

    pairs = deal(
        [jnp.concatenate([pick(expert_gate, k), pick(expert_up, k)], axis=1) for k in range(tp)]
    )
    downs = deal([pick(expert_down, k) for k in range(tp)])

    spread, pick0, pick1 = call(
        functools.partial(route_kernel, experts, cap),
        [
            jax.ShapeDtypeStruct((experts * cap, tok), BF16),
            jax.ShapeDtypeStruct((tok, experts * cap), BF16),
            jax.ShapeDtypeStruct((tok, experts * cap), BF16),
        ],
        (routes.T,),
    )
    gain = norm_gain.astype(F32).reshape(tp, 1, width)

    mixed = call(
        functools.partial(attn_kernel, nz, tok),
        [jax.ShapeDtypeStruct((half, 128), BF16)] * nz,
        (core_ref, z_ref, *owns, *swapped),
        smem=2,
        scratch=(
            pltpu.VMEM((nz, 2 * tok, 128), BF16),
            pltpu.VMEM((nz, 2 * tok, 128), BF16),
            pltpu.VMEM((nz, 8, 2 * tok), F32),
            pltpu.VMEM((nz, half, 128), BF16),
            pltpu.VMEM((nz, half, 128), BF16),
        ),
    )
    back = [mixed[0]] + [over_z(mixed[k], k) for k in range(1, nz)]
    attended = jnp.stack(back)
    attended_all = all_tp(attended)
    mid, outgoing = call(
        functools.partial(mid_kernel, heads, cap),
        [
            jax.ShapeDtypeStruct((tok, width), BF16),
            jax.ShapeDtypeStruct((experts, cap, width), BF16),
        ],
        (me_ref, z_ref, *attended_all, out_weight, residual, spread),
        smem=2,
    )
    arrived = lax.all_to_all(outgoing, ("sp", "tp"), 0, 0, tiled=True)
    mids = all_tp(mid)
    produced = call(
        functools.partial(expert_kernel, sp, tp),
        jax.ShapeDtypeStruct((sp * tp, cap, width), BF16),
        (me_ref, arrived, gain, *pairs, *downs),
        smem=1,
        scratch=(
            pltpu.VMEM((sp * cap, tp * width), BF16),
            pltpu.VMEM((sp * cap, tp * expert_gate.shape[2]), BF16),
        ),
    )
    returned = lax.all_to_all(produced, ("sp", "tp"), 0, 0, tiled=True)
    shared_mid = call(
        shared_kernel,
        jax.ShapeDtypeStruct((tok, shared_gate.shape[1]), BF16),
        (me_ref, *mids, gain, shared_gate, shared_up),
        smem=1,
    )
    shared_mids = all_tp(shared_mid)
    return call(
        final_kernel,
        jax.ShapeDtypeStruct((tok, width), BF16),
        (me_ref, *shared_mids, shared_down, mid, returned, pick0, pick1, route_weight.T),
        smem=1,
        scratch=(pltpu.VMEM((tok, shared_down.shape[0]), BF16),),
    )


def slot_targets(routes, experts_all, capacity):
    flat_routes = routes.reshape(-1)
    onehot = (flat_routes[:, None] == jnp.arange(experts_all, dtype=jnp.int32)[None, :]).astype(
        jnp.int32
    )
    before = jnp.cumsum(onehot, axis=0) - onehot
    return flat_routes * capacity + jnp.sum(before * onehot, axis=1)


def keep_state(fold_state):
    return fold_state


def generic_shards(
    queries,
    key_vectors,
    value_vectors,
    log_gate_sums,
    residual,
    out_weight,
    norm_gain,
    routes,
    route_weight,
    expert_gate,
    expert_up,
    expert_down,
    shared_gate,
    shared_up,
    shared_down,
):
    tok_dev = queries.shape[0]
    head_dim = HDIM
    local_heads = log_gate_sums.shape[1]
    local_width = residual.shape[1]
    model_width = norm_gain.shape[0]
    score_scale = head_dim ** (-0.5)
    seq_first = lax.axis_index("sp") * tok_dev
    query_heads = queries.reshape(tok_dev, local_heads, head_dim)
    query_pos = seq_first + jnp.arange(tok_dev, dtype=jnp.int32)
    own_gates = log_gate_sums.T
    all_gates = lax.all_gather(log_gate_sums, "sp", axis=0, tiled=True)
    initial = (
        jnp.full((local_heads, tok_dev), -1e30, jnp.float32),
        jnp.zeros((local_heads, tok_dev), jnp.float32),
        jnp.zeros((local_heads, tok_dev, head_dim), jnp.float32),
    )
    key_heads = key_vectors.reshape(tok_dev, local_heads, head_dim)
    value_heads = value_vectors.reshape(tok_dev, local_heads, head_dim)
    key_part = lax.all_gather(key_heads, "sp", axis=0, tiled=True)
    value_part = lax.all_gather(value_heads, "sp", axis=0, tiled=True)
    part_rows = key_part.shape[0]
    block_size = math.gcd(part_rows, 512)
    key_blocks = key_part.reshape(part_rows // block_size, block_size, local_heads, head_dim)
    value_blocks = value_part.reshape(part_rows // block_size, block_size, local_heads, head_dim)

    def one_block(fold_state, inputs):
        key_block, value_block, block_number = inputs
        block_first = block_number * block_size

        def compute(old_state):
            running_max, weight_total, summed = old_state
            gate_block = lax.dynamic_slice_in_dim(all_gates, block_first, block_size, 0).T
            scores = (
                jnp.einsum(
                    "qhd,khd->hqk", query_heads, key_block, preferred_element_type=jnp.float32
                )
                * score_scale
            )
            scores = scores + own_gates[:, :, None] - gate_block[:, None, :]
            key_pos = block_first + jnp.arange(block_size, dtype=jnp.int32)
            allowed = (key_pos[None, :] <= query_pos[:, None])[None]
            newmax = jnp.maximum(running_max, jnp.max(jnp.where(allowed, scores, -jnp.inf), axis=2))
            factor = jnp.exp(running_max - newmax)
            weight = jnp.where(allowed, jnp.exp(scores - newmax[:, :, None]), 0.0)
            weight_total = weight_total * factor + jnp.sum(weight, axis=2)
            summed = summed * factor[:, :, None] + jnp.einsum(
                "hqk,khd->hqd",
                weight.astype(jnp.bfloat16),
                value_block,
                preferred_element_type=jnp.float32,
            )
            return (newmax, weight_total, summed)

        useful = block_first <= seq_first + tok_dev - 1
        return (lax.cond(useful, compute, keep_state, fold_state), None)

    numbers = jnp.arange(part_rows // block_size, dtype=jnp.int32)
    result_state, _ = lax.scan(one_block, initial, (key_blocks, value_blocks, numbers))
    _, weight_total, summed = result_state
    attended = (summed / weight_total[:, :, None]).astype(jnp.bfloat16)
    attended = attended.transpose(1, 0, 2).reshape(tok_dev, local_heads * head_dim)
    weight_rows = out_weight
    projected = jnp.dot(
        lax.all_gather(attended, "tp", axis=1, tiled=True),
        weight_rows,
        preferred_element_type=jnp.float32,
    )
    mid = (residual.astype(jnp.float32) + projected).astype(jnp.bfloat16)
    mid_wide = mid.astype(jnp.float32)
    feature_first = lax.axis_index("tp") * local_width
    squares = lax.psum(jnp.sum(mid_wide * mid_wide, axis=1), "tp")
    inverse = lax.rsqrt(squares / model_width + EPSILON)
    own_gain = lax.dynamic_slice_in_dim(norm_gain, feature_first, local_width, 0).astype(
        jnp.float32
    )
    normed_own = (mid_wide * inverse[:, None] * own_gain[None, :]).astype(jnp.bfloat16)
    normed = lax.all_gather(normed_own, "tp", axis=1, tiled=True)
    shared_mid = silu_gate(
        jnp.dot(normed, shared_gate, preferred_element_type=jnp.float32),
        jnp.dot(normed, shared_up, preferred_element_type=jnp.float32),
    ).astype(jnp.bfloat16)
    weight_rows = shared_down
    shared_out = jnp.dot(
        lax.all_gather(shared_mid, "tp", axis=1, tiled=True),
        weight_rows,
        preferred_element_type=jnp.float32,
    )
    exp_dev = expert_gate.shape[0]
    sp_count = lax.axis_size("sp")
    experts_all = exp_dev * sp_count
    top_count = routes.shape[1]
    capacity = 5 * tok_dev * top_count // (4 * experts_all)
    targets = slot_targets(routes, experts_all, capacity)
    owners = (
        jnp.full((experts_all * capacity,), tok_dev, jnp.int32)
        .at[targets]
        .set(jnp.arange(tok_dev * top_count, dtype=jnp.int32) // top_count)
    )
    padded = jnp.concatenate(
        [normed_own, jnp.zeros((1, normed_own.shape[1]), jnp.bfloat16)], axis=0
    )
    outgoing = padded[owners].reshape(sp_count, exp_dev, capacity, normed_own.shape[1])
    rows_all = lax.all_gather(
        lax.all_to_all(outgoing, "sp", split_axis=0, concat_axis=0, tiled=True),
        "tp",
        axis=3,
        tiled=True,
    )
    gate_part = jnp.einsum(
        "secd,edf->secf", rows_all, expert_gate, preferred_element_type=jnp.float32
    )
    up_part = jnp.einsum("secd,edf->secf", rows_all, expert_up, preferred_element_type=jnp.float32)
    hidden = silu_gate(gate_part, up_part).astype(jnp.bfloat16)
    hidden_all = lax.all_gather(hidden, "tp", axis=3, tiled=True)
    produced = jnp.einsum(
        "secf,efd->secd", hidden_all, expert_down, preferred_element_type=jnp.float32
    ).astype(jnp.bfloat16)
    returned = lax.all_to_all(produced, "sp", split_axis=0, concat_axis=0, tiled=True)
    returned_flat = returned.reshape(experts_all * capacity, local_width)
    picked = returned_flat[targets].astype(jnp.float32).reshape(tok_dev, top_count, local_width)
    routed = jnp.sum(picked * route_weight[:, :, None], axis=1)
    return (mid_wide + shared_out + routed).astype(jnp.bfloat16)


def layer(*args):
    return shards(*args)


def solution(mesh):
    placed = (
        P("sp", "tp"),
        P("sp", "tp"),
        P("sp", "tp"),
        P("sp", "tp"),
        P("sp", "tp"),
        P(None, "tp"),
        P(),
        P("sp", None),
        P("sp", None),
        P("sp", None, "tp"),
        P("sp", None, "tp"),
        P("sp", None, "tp"),
        P(None, "tp"),
        P(None, "tp"),
        P(None, "tp"),
    )
    sp, tp = mesh.shape["sp"], mesh.shape["tp"]

    def program(*args):
        heads = args[3].shape[1] // tp
        exp_dev = args[9].shape[0] // sp
        deals = sp % 2 == 0 and heads * 2 == sp and exp_dev == tp and tp & (tp - 1) == 0
        body = layer if deals else generic_shards
        mapped = jax.shard_map(body, mesh=mesh, in_specs=placed, out_specs=P("sp", "tp"), check_vma=False)
        return mapped(*args)

    return program
```

```python
import functools
import math

import jax
import jax.numpy as jnp
from jax import lax
from jax.experimental import pallas as pl
from jax.experimental.pallas import tpu as pltpu
from jax.sharding import PartitionSpec as P


HDIM = 64
EPSILON = 1e-06
LOG2E = math.log2(math.e)
LOW = -1e30
VMEM_GRANT = 24 * 2**20
F32 = jnp.float32
BF16 = jnp.bfloat16


def silu_gate(gate_part, up_part):
    return jax.nn.silu(gate_part) * up_part


def call(kernel, out_shape, args, smem=0, scratch=(), far_in=0):
    vm = pl.BlockSpec(memory_space=pltpu.VMEM)
    sm = pl.BlockSpec(memory_space=pltpu.SMEM)
    far = pl.BlockSpec(memory_space=pl.ANY)
    single = not isinstance(out_shape, (list, tuple))
    return pl.pallas_call(
        kernel,
        out_shape=out_shape,
        in_specs=[sm] * smem + [vm] * (len(args) - smem - far_in) + [far] * far_in,
        out_specs=vm if single else [vm] * len(out_shape),
        scratch_shapes=list(scratch),
        compiler_params=pltpu.CompilerParams(vmem_limit_bytes=None if far_in else VMEM_GRANT),
    )(*args)


def low_lanes(shape):
    return lax.broadcasted_iota(jnp.int32, shape, 1) < HDIM


def swap_halves(x):
    return pltpu.roll(x, HDIM, 1)


def cut_copies(sources, sems):
    copies = []
    for src, index, dst, cols in sources:
        dst = dst if cols is None else dst.at[:, cols]
        copy = pltpu.make_async_copy(src.at[index], dst, sems.at[len(copies)])
        copy.start()
        copies.append(copy)
    return copies


def pair_sources(gate_ref, up_ref, index, dst):
    hid = gate_ref.shape[2]
    return [(gate_ref, index, dst, slice(0, hid)), (up_ref, index, dst, slice(hid, 2 * hid))]


def cut_pairs_kernel(offsets, t_ref, gate_ref, up_ref, *refs):
    sources = []
    for offset, dst in zip(offsets, refs[:-1]):
        sources += pair_sources(gate_ref, up_ref, t_ref[0] ^ offset, dst)
    for copy in cut_copies(sources, refs[-1]):
        copy.wait()


def cut_downs_kernel(offsets, t_ref, down_ref, *refs):
    sources = [(down_ref, t_ref[0] ^ offset, dst, None) for offset, dst in zip(offsets, refs[:-1])]
    for copy in cut_copies(sources, refs[-1]):
        copy.wait()


def pack_kernel(heads, offset, z_ref, t_ref, q_ref, k_ref, v_ref, g_ref, gate_ref, up_ref, down_ref, *refs):
    tok = q_ref.shape[0]
    half = tok // 2
    low = low_lanes((tok, 2 * HDIM))
    low_half = low_lanes((half, 2 * HDIM))
    slabs, (pair_ref, cut_ref, o_ref, sems) = refs[:heads], refs[heads:]
    other = t_ref[0] ^ offset
    sources = pair_sources(gate_ref, up_ref, other, pair_ref) + [(down_ref, other, cut_ref, None)]
    copies = cut_copies(sources, sems)
    gates = g_ref[...]
    for pair in range(heads // 2):
        cols = slice(pair * 2 * HDIM, (pair + 1) * 2 * HDIM)
        q = q_ref[:, cols].astype(F32)
        k = k_ref[:, cols].astype(F32)
        v = v_ref[:, cols].astype(F32)
        o_ref[2 * pair, 0:tok] = jnp.where(low, k, swap_halves(v)).astype(BF16)
        o_ref[2 * pair + 1, 0:tok] = jnp.where(low, swap_halves(k), v).astype(BF16)
        qa, qb = q[:half], q[half:]
        o_ref[2 * pair, tok : tok + half] = jnp.where(low_half, qa, swap_halves(qb)).astype(BF16)
        o_ref[2 * pair + 1, tok : tok + half] = jnp.where(low_half, swap_halves(qa), qb).astype(BF16)
    rows = tok // 128
    for h in range(heads):
        left = gates[h : h + 1]
        pieces = []
        for _ in range(3):
            piece = left.astype(BF16).astype(F32)
            left = left - piece
            pieces += [piece[:, r * 128 : (r + 1) * 128] for r in range(rows)]
        pad = o_ref.shape[1] - tok - half - len(pieces)
        pieces.append(jnp.zeros((pad, 128), F32))
        o_ref[h, tok + half :] = jnp.concatenate(pieces, axis=0).astype(BF16)
    for i, slab in enumerate(slabs):
        slab[...] = o_ref[z_ref[0] ^ i]
    for copy in copies:
        copy.wait()


def attn_kernel(nz, tok, ahead, parts, c_ref, z_ref, *refs):
    owns, sws, outs = refs[:nz], refs[nz : 2 * nz], refs[2 * nz : 3 * nz]
    kv_scr, vo_scr, g_scr, q_scr, o_scr = refs[3 * nz :]
    core = c_ref[0]
    half = tok // 2
    wide = 2 * tok
    rows = tok // 128
    n = half // parts
    low_tok = low_lanes((tok, 128))
    low_half = low_lanes((half, 128))
    for i in range(nz):
        z = z_ref[0] ^ i
        q_scr[z] = owns[i][tok : tok + half]
        for ref, at in ((owns[i], core), (sws[i], 1 - core)):
            kv = ref[0:tok]
            spot = pl.ds(pl.multiple_of(at * tok, tok), tok)
            kv_scr[z, spot] = kv
            vo_scr[z, spot] = jnp.where(low_tok, 1.0, kv.astype(F32)).astype(BF16)
            g = ref[tok + half :].astype(F32)
            g = (g[0:rows] + g[rows : 2 * rows] + g[2 * rows : 3 * rows]) * LOG2E
            g = jnp.concatenate([g[r : r + 1] for r in range(rows)], axis=1)
            g_scr[z, 0:1, spot] = g
    scale = HDIM ** (-0.5) * LOG2E
    key_at = lax.broadcasted_iota(jnp.int32, (n, wide), 1)
    row_at = lax.broadcasted_iota(jnp.int32, (n, wide), 0) + core * tok
    low = low_lanes((n, 128))
    queries = {}
    state = {}

    def query(zq, i):
        if zq not in queries:
            packed = q_scr[zq].astype(F32)
            queries[zq] = (
                jnp.where(low_half, packed, 0.0).astype(BF16),
                jnp.where(low_half, swap_halves(packed), 0.0).astype(BF16),
            )
        return queries[zq][i]

    def seen(zq, z, i, p):
        return wide if z < zq else tok + i * half + (p + 1) * n

    def score(zq, z, i, p):
        keys = kv_scr[z, 0 : seen(zq, z, i, p)]
        q = query(zq, i)[p * n : (p + 1) * n]
        return lax.dot_general(q, keys, (((1,), (1,)), ((), ())), preferred_element_type=F32)

    def absorb(zq, z, i, p, s):
        keys = seen(zq, z, i, p)
        t = s * scale - g_scr[z, 0:1, 0:keys]
        if z == zq:
            t = jnp.where(key_at[:, :keys] <= row_at[:, :keys] + (i * half + p * n), t, LOW)
        top = jnp.max(t, axis=1, keepdims=True)
        if z > 0:
            m, acc = state[zq, i, p]
            top = jnp.maximum(m, top)
        weight = jnp.exp2(t - top).astype(BF16)
        new = jnp.dot(weight, vo_scr[z, 0:keys], preferred_element_type=F32)
        if z > 0:
            new = new + acc * jnp.exp2(m - top)
        state[zq, i, p] = top, new
        if z == zq and i == 1:
            first = state[zq, 0, p][1]
            out = jnp.where(low, swap_halves(first) / first, new / swap_halves(new))
            o_scr[zq, p * n : (p + 1) * n] = out.astype(BF16)

    tasks = [(zq, z, i, p) for zq in range(nz) for z in range(zq + 1) for i in range(2) for p in range(parts)]
    scores = [score(*task) for task in tasks[:ahead]]
    for at, task in enumerate(tasks):
        if at + ahead < len(tasks):
            scores.append(score(*tasks[at + ahead]))
        absorb(*task, scores.pop(0))
    for i in range(nz):
        outs[i][...] = o_scr[z_ref[0] ^ i]


def route_kernel(experts, cap, rt_ref, w_ref, d_ref, c_ref):
    tok = rt_ref.shape[1]
    slots = experts * cap
    at = lax.broadcasted_iota(jnp.int32, (tok, tok), 0)
    bt = lax.broadcasted_iota(jnp.int32, (tok, tok), 1)
    eid = lax.broadcasted_iota(jnp.int32, (experts, tok), 0)
    hot = [jnp.where(eid == rt_ref[k : k + 1], 1.0, 0.0) for k in range(2)]
    before = jnp.where(at < bt, 1.0, 0.0).astype(BF16)
    rank = jnp.dot((hot[0] + hot[1]).astype(BF16), before, preferred_element_type=F32)
    place = rank + (eid * cap).astype(F32)
    rows = [jnp.sum(h * place, axis=0, keepdims=True).astype(jnp.int32) for h in hot]
    sid = lax.broadcasted_iota(jnp.int32, (slots, tok), 0)
    d_ref[...] = jnp.where((sid == rows[0]) | (sid == rows[1]), 1.0, 0.0).astype(BF16)
    cols = jnp.concatenate([r.astype(F32) for r in rows] * 4, axis=0).T.astype(jnp.int32)
    w = jnp.concatenate([w_ref[...]] * 4, axis=0).T
    cols = [cols[:, k : k + 1] for k in range(2)]
    sid = lax.broadcasted_iota(jnp.int32, (tok, slots), 1)
    mix = jnp.where(sid == cols[0], w[:, 0:1], jnp.where(sid == cols[1], w[:, 1:2], 0.0))
    c_ref[...] = mix.astype(BF16)


def mid_kernel(heads, cap, t_ref, z_ref, *refs):
    n = len(refs) - 5
    parts, (w_ref, r_ref, d_ref, m_ref, out_ref) = refs[:n], refs[n:]
    half = parts[0].shape[1]
    width = heads * HDIM
    low = low_lanes((half, 2 * HDIM))
    tops = [None, None]
    for k in range(n):
        src = t_ref[0] ^ k
        w = w_ref[pl.ds(pl.multiple_of(src * width, width), width), :]
        ab = ([], [])
        for pair in range(heads // 2):
            p0 = parts[k][z_ref[0] ^ (2 * pair)].astype(F32)
            p1 = parts[k][z_ref[0] ^ (2 * pair + 1)].astype(F32)
            ab[0].append(jnp.where(low, p0, swap_halves(p1)).astype(BF16))
            ab[1].append(jnp.where(low, swap_halves(p0), p1).astype(BF16))
        for i in range(2):
            got = jnp.dot(jnp.concatenate(ab[i], axis=1), w, preferred_element_type=F32)
            tops[i] = got if tops[i] is None else tops[i] + got
    for i in range(2):
        rows = slice(i * half, (i + 1) * half)
        m_ref[rows] = (r_ref[rows].astype(F32) + tops[i]).astype(BF16)
    mid = m_ref[...]
    experts = out_ref.shape[0]
    group = 4
    for e in range(0, experts, group):
        got = jnp.dot(d_ref[e * cap : (e + group) * cap], mid, preferred_element_type=F32)
        for i in range(group):
            out_ref[e + i] = got[i * cap : (i + 1) * cap].astype(BF16)


def normed_of(parts, gains, width):
    total = None
    for x in parts:
        sq = jnp.sum(x * x, axis=1, keepdims=True)
        total = sq if total is None else total + sq
    inverse = lax.rsqrt(total / width + EPSILON)
    return [(x * inverse * g).astype(BF16) for x, g in zip(parts, gains)]


def shared_kernel(t_ref, *refs):
    n = len(refs) - 5
    parts, halves, (gain_ref, gate_ref, up_ref, o_ref) = refs[: n - 1], refs[n - 1 : n + 1], refs[n + 1 :]
    part_width = parts[0].shape[1]
    width = n * part_width
    srcs = [t_ref[0] ^ k for k in range(n)]
    rows = [p[...].astype(F32) for p in parts]
    rows.append(jnp.concatenate([h[...].astype(F32) for h in halves], axis=0))
    normed = normed_of(rows, [gain_ref[s] for s in srcs], width)
    both = None
    for s, x in zip(srcs, normed):
        rows = pl.ds(pl.multiple_of(s * part_width, part_width), part_width)
        w = jnp.concatenate([gate_ref[rows, :], up_ref[rows, :]], axis=1)
        got = jnp.dot(x, w, preferred_element_type=F32)
        both = got if both is None else both + got
    hid = gate_ref.shape[1]
    o_ref[...] = silu_gate(both[:, :hid], both[:, hid:]).astype(BF16)


def expert_kernel(sp, tp, t_ref, x_ref, gain_ref, *refs):
    pairs, downs = refs[:tp], refs[tp : 2 * tp]
    y_ref, x_scr, h_scr = refs[2 * tp :]
    me = t_ref[0]
    cap, part_width = x_ref.shape[1:]
    parts = [
        jnp.concatenate([x_ref[s * tp + t].astype(F32) for s in range(sp)], axis=0) for t in range(tp)
    ]
    normed = normed_of(parts, [gain_ref[t] for t in range(tp)], tp * part_width)
    for t in range(tp):
        x_scr[:, t * part_width : (t + 1) * part_width] = normed[t]
    x = x_scr[...]
    hid = pairs[0].shape[1] // 2
    for k in range(tp):
        both = jnp.dot(x, pairs[k][...], preferred_element_type=F32)
        spot = pl.ds(pl.multiple_of((me ^ k) * hid, hid), hid)
        h_scr[:, spot] = silu_gate(both[:, :hid], both[:, hid:]).astype(BF16)
    h = h_scr[...]
    for k in range(tp):
        y = jnp.dot(h, downs[k][...], preferred_element_type=F32)
        for s in range(sp):
            y_ref[s * tp + (me ^ k)] = y[s * cap : (s + 1) * cap].astype(BF16)


def picks_kernel(mid_ref, ret_ref, c_ref, o_ref):
    experts, cap, width = ret_ref.shape
    rows = ret_ref[...].astype(F32).reshape(experts * cap, width).astype(BF16)
    o_ref[...] = mid_ref[...].astype(F32) + jnp.dot(c_ref[...], rows, preferred_element_type=F32)


def final_kernel(t_ref, *refs):
    n = len(refs) - 4
    hids = refs[:n]
    down_ref, sum_ref, o_ref, h_scr = refs[n:]
    hid = hids[0].shape[1]
    for k in range(n):
        spot = pl.ds(pl.multiple_of((t_ref[0] ^ k) * hid, hid), hid)
        h_scr[:, spot] = hids[k][...]
    out = jnp.dot(h_scr[...], down_ref[...], preferred_element_type=F32)
    o_ref[...] = (sum_ref[...] + out).astype(BF16)


def shards(
    queries,
    key_vectors,
    value_vectors,
    log_gate_sums,
    residual,
    out_weight,
    norm_gain,
    routes,
    route_weight,
    expert_gate,
    expert_up,
    expert_down,
    shared_gate,
    shared_up,
    shared_down,
):
    sp, tp = lax.axis_size("sp"), lax.axis_size("tp")
    tok = queries.shape[0]
    heads = log_gate_sums.shape[1]
    width = residual.shape[1]
    exp_dev = expert_gate.shape[0]
    experts = exp_dev * sp
    top_count = routes.shape[1]
    cap = 5 * tok * top_count // (4 * experts)
    nz = sp // 2
    me = lax.axis_index("tp")
    me_ref = me.astype(jnp.int32).reshape(1)
    core_ref = (lax.axis_index("sp") % 2).astype(jnp.int32).reshape(1)
    half = tok // 2
    rows = tok + half + -(-3 * (tok // 128) // 16) * 16

    def over_tp(x, k):
        return lax.ppermute(x, "tp", [(i, i ^ k) for i in range(tp)])

    def all_tp(x):
        return [x] + [over_tp(x, k) for k in range(1, tp)]

    z = lax.axis_index("sp") // 2
    z_ref = z.astype(jnp.int32).reshape(1)

    def over_z(x, k):
        return lax.ppermute(x, "sp", [(i, i ^ (2 * k)) for i in range(sp)])

    pair_shape = jax.ShapeDtypeStruct((expert_gate.shape[1], 2 * expert_gate.shape[2]), BF16)
    down_shape = jax.ShapeDtypeStruct(expert_down.shape[1:], BF16)
    *slabs, far_pair, far_down = call(
        functools.partial(pack_kernel, heads, tp - 1),
        [jax.ShapeDtypeStruct((rows, 128), BF16)] * heads + [pair_shape, down_shape],
        (z_ref, me_ref, queries, key_vectors, value_vectors, log_gate_sums.T)
        + (expert_gate, expert_up, expert_down),
        smem=2,
        scratch=(pltpu.VMEM((heads, rows, 128), BF16), pltpu.SemaphoreType.DMA((3,))),
        far_in=3,
    )
    owns = [slabs[0]] + [over_z(slabs[k], k) for k in range(1, nz)]
    swapped = [lax.ppermute(x, "sp", [(i, i ^ 1) for i in range(sp)]) for x in owns]

    near = tuple(range(tp - 1))
    near_downs = call(
        functools.partial(cut_downs_kernel, near),
        [down_shape] * len(near),
        (me_ref, expert_down),
        smem=1,
        scratch=(pltpu.SemaphoreType.DMA((len(near),)),),
        far_in=1,
    )
    near_pairs = call(
        functools.partial(cut_pairs_kernel, near),
        [pair_shape] * len(near),
        (me_ref, expert_gate, expert_up),
        smem=1,
        scratch=(pltpu.SemaphoreType.DMA((2 * len(near),)),),
        far_in=2,
    )
    pairs = [near_pairs[0]] + [over_tp(near_pairs[k], k) for k in near[1:]]
    downs = [near_downs[0]] + [over_tp(near_downs[k], k) for k in near[1:]]
    pairs.append(over_tp(far_pair, tp - 1))
    downs.append(over_tp(far_down, tp - 1))

    spread, mix = call(
        functools.partial(route_kernel, experts, cap),
        [
            jax.ShapeDtypeStruct((experts * cap, tok), BF16),
            jax.ShapeDtypeStruct((tok, experts * cap), BF16),
        ],
        (routes.T, route_weight.T),
    )
    gain = norm_gain.astype(F32).reshape(tp, 1, width)

    mixed = call(
        functools.partial(attn_kernel, nz, tok, 2, 2),
        [jax.ShapeDtypeStruct((half, 128), BF16)] * nz,
        (core_ref, z_ref, *owns, *swapped),
        smem=2,
        scratch=(
            pltpu.VMEM((nz, 2 * tok, 128), BF16),
            pltpu.VMEM((nz, 2 * tok, 128), BF16),
            pltpu.VMEM((nz, 8, 2 * tok), F32),
            pltpu.VMEM((nz, half, 128), BF16),
            pltpu.VMEM((nz, half, 128), BF16),
        ),
    )
    back = [mixed[0]] + [over_z(mixed[k], k) for k in range(1, nz)]
    attended = jnp.stack(back)
    attended_all = all_tp(attended)
    mid, outgoing = call(
        functools.partial(mid_kernel, heads, cap),
        [
            jax.ShapeDtypeStruct((tok, width), BF16),
            jax.ShapeDtypeStruct((experts, cap, width), BF16),
        ],
        (me_ref, z_ref, *attended_all, out_weight, residual, spread),
        smem=2,
    )
    arrived = lax.all_to_all(outgoing, ("sp", "tp"), 0, 0, tiled=True)
    mids = [mid] + [over_tp(mid, k) for k in range(1, tp - 1)]
    mids += [over_tp(mids[2][:half], 1), over_tp(mids[1][half:], 2)]
    produced = call(
        functools.partial(expert_kernel, sp, tp),
        jax.ShapeDtypeStruct((sp * tp, cap, width), BF16),
        (me_ref, arrived, gain, *pairs, *downs),
        smem=1,
        scratch=(
            pltpu.VMEM((sp * cap, tp * width), BF16),
            pltpu.VMEM((sp * cap, tp * expert_gate.shape[2]), BF16),
        ),
    )
    returned = lax.all_to_all(produced, ("sp", "tp"), 0, 0, tiled=True)
    shared_mid = call(
        shared_kernel,
        jax.ShapeDtypeStruct((tok, shared_gate.shape[1]), BF16),
        (me_ref, *mids, gain, shared_gate, shared_up),
        smem=1,
    )
    shared_mids = all_tp(shared_mid)
    summed = call(picks_kernel, jax.ShapeDtypeStruct((tok, width), F32), (mid, returned, mix))
    return call(
        final_kernel,
        jax.ShapeDtypeStruct((tok, width), BF16),
        (me_ref, *shared_mids, shared_down, summed),
        smem=1,
        scratch=(pltpu.VMEM((tok, shared_down.shape[0]), BF16),),
    )


def slot_targets(routes, experts_all, capacity):
    flat_routes = routes.reshape(-1)
    onehot = (flat_routes[:, None] == jnp.arange(experts_all, dtype=jnp.int32)[None, :]).astype(
        jnp.int32
    )
    before = jnp.cumsum(onehot, axis=0) - onehot
    return flat_routes * capacity + jnp.sum(before * onehot, axis=1)


def keep_state(fold_state):
    return fold_state


def generic_shards(
    queries,
    key_vectors,
    value_vectors,
    log_gate_sums,
    residual,
    out_weight,
    norm_gain,
    routes,
    route_weight,
    expert_gate,
    expert_up,
    expert_down,
    shared_gate,
    shared_up,
    shared_down,
):
    tok_dev = queries.shape[0]
    head_dim = HDIM
    local_heads = log_gate_sums.shape[1]
    local_width = residual.shape[1]
    model_width = norm_gain.shape[0]
    score_scale = head_dim ** (-0.5)
    seq_first = lax.axis_index("sp") * tok_dev
    query_heads = queries.reshape(tok_dev, local_heads, head_dim)
    query_pos = seq_first + jnp.arange(tok_dev, dtype=jnp.int32)
    own_gates = log_gate_sums.T
    all_gates = lax.all_gather(log_gate_sums, "sp", axis=0, tiled=True)
    initial = (
        jnp.full((local_heads, tok_dev), -1e30, jnp.float32),
        jnp.zeros((local_heads, tok_dev), jnp.float32),
        jnp.zeros((local_heads, tok_dev, head_dim), jnp.float32),
    )
    key_heads = key_vectors.reshape(tok_dev, local_heads, head_dim)
    value_heads = value_vectors.reshape(tok_dev, local_heads, head_dim)
    key_part = lax.all_gather(key_heads, "sp", axis=0, tiled=True)
    value_part = lax.all_gather(value_heads, "sp", axis=0, tiled=True)
    part_rows = key_part.shape[0]
    block_size = math.gcd(part_rows, 512)
    key_blocks = key_part.reshape(part_rows // block_size, block_size, local_heads, head_dim)
    value_blocks = value_part.reshape(part_rows // block_size, block_size, local_heads, head_dim)

    def one_block(fold_state, inputs):
        key_block, value_block, block_number = inputs
        block_first = block_number * block_size

        def compute(old_state):
            running_max, weight_total, summed = old_state
            gate_block = lax.dynamic_slice_in_dim(all_gates, block_first, block_size, 0).T
            scores = (
                jnp.einsum(
                    "qhd,khd->hqk", query_heads, key_block, preferred_element_type=jnp.float32
                )
                * score_scale
            )
            scores = scores + own_gates[:, :, None] - gate_block[:, None, :]
            key_pos = block_first + jnp.arange(block_size, dtype=jnp.int32)
            allowed = (key_pos[None, :] <= query_pos[:, None])[None]
            newmax = jnp.maximum(running_max, jnp.max(jnp.where(allowed, scores, -jnp.inf), axis=2))
            factor = jnp.exp(running_max - newmax)
            weight = jnp.where(allowed, jnp.exp(scores - newmax[:, :, None]), 0.0)
            weight_total = weight_total * factor + jnp.sum(weight, axis=2)
            summed = summed * factor[:, :, None] + jnp.einsum(
                "hqk,khd->hqd",
                weight.astype(jnp.bfloat16),
                value_block,
                preferred_element_type=jnp.float32,
            )
            return (newmax, weight_total, summed)

        useful = block_first <= seq_first + tok_dev - 1
        return (lax.cond(useful, compute, keep_state, fold_state), None)

    numbers = jnp.arange(part_rows // block_size, dtype=jnp.int32)
    result_state, _ = lax.scan(one_block, initial, (key_blocks, value_blocks, numbers))
    _, weight_total, summed = result_state
    attended = (summed / weight_total[:, :, None]).astype(jnp.bfloat16)
    attended = attended.transpose(1, 0, 2).reshape(tok_dev, local_heads * head_dim)
    weight_rows = out_weight
    projected = jnp.dot(
        lax.all_gather(attended, "tp", axis=1, tiled=True),
        weight_rows,
        preferred_element_type=jnp.float32,
    )
    mid = (residual.astype(jnp.float32) + projected).astype(jnp.bfloat16)
    mid_wide = mid.astype(jnp.float32)
    feature_first = lax.axis_index("tp") * local_width
    squares = lax.psum(jnp.sum(mid_wide * mid_wide, axis=1), "tp")
    inverse = lax.rsqrt(squares / model_width + EPSILON)
    own_gain = lax.dynamic_slice_in_dim(norm_gain, feature_first, local_width, 0).astype(
        jnp.float32
    )
    normed_own = (mid_wide * inverse[:, None] * own_gain[None, :]).astype(jnp.bfloat16)
    normed = lax.all_gather(normed_own, "tp", axis=1, tiled=True)
    shared_mid = silu_gate(
        jnp.dot(normed, shared_gate, preferred_element_type=jnp.float32),
        jnp.dot(normed, shared_up, preferred_element_type=jnp.float32),
    ).astype(jnp.bfloat16)
    weight_rows = shared_down
    shared_out = jnp.dot(
        lax.all_gather(shared_mid, "tp", axis=1, tiled=True),
        weight_rows,
        preferred_element_type=jnp.float32,
    )
    exp_dev = expert_gate.shape[0]
    sp_count = lax.axis_size("sp")
    experts_all = exp_dev * sp_count
    top_count = routes.shape[1]
    capacity = 5 * tok_dev * top_count // (4 * experts_all)
    targets = slot_targets(routes, experts_all, capacity)
    owners = (
        jnp.full((experts_all * capacity,), tok_dev, jnp.int32)
        .at[targets]
        .set(jnp.arange(tok_dev * top_count, dtype=jnp.int32) // top_count)
    )
    padded = jnp.concatenate(
        [normed_own, jnp.zeros((1, normed_own.shape[1]), jnp.bfloat16)], axis=0
    )
    outgoing = padded[owners].reshape(sp_count, exp_dev, capacity, normed_own.shape[1])
    rows_all = lax.all_gather(
        lax.all_to_all(outgoing, "sp", split_axis=0, concat_axis=0, tiled=True),
        "tp",
        axis=3,
        tiled=True,
    )
    gate_part = jnp.einsum(
        "secd,edf->secf", rows_all, expert_gate, preferred_element_type=jnp.float32
    )
    up_part = jnp.einsum("secd,edf->secf", rows_all, expert_up, preferred_element_type=jnp.float32)
    hidden = silu_gate(gate_part, up_part).astype(jnp.bfloat16)
    hidden_all = lax.all_gather(hidden, "tp", axis=3, tiled=True)
    produced = jnp.einsum(
        "secf,efd->secd", hidden_all, expert_down, preferred_element_type=jnp.float32
    ).astype(jnp.bfloat16)
    returned = lax.all_to_all(produced, "sp", split_axis=0, concat_axis=0, tiled=True)
    returned_flat = returned.reshape(experts_all * capacity, local_width)
    picked = returned_flat[targets].astype(jnp.float32).reshape(tok_dev, top_count, local_width)
    routed = jnp.sum(picked * route_weight[:, :, None], axis=1)
    return (mid_wide + shared_out + routed).astype(jnp.bfloat16)


def layer(*args):
    return shards(*args)


def solution(mesh):
    placed = (
        P("sp", "tp"),
        P("sp", "tp"),
        P("sp", "tp"),
        P("sp", "tp"),
        P("sp", "tp"),
        P(None, "tp"),
        P(),
        P("sp", None),
        P("sp", None),
        P("sp", None, "tp"),
        P("sp", None, "tp"),
        P("sp", None, "tp"),
        P(None, "tp"),
        P(None, "tp"),
        P(None, "tp"),
    )
    sp, tp = mesh.shape["sp"], mesh.shape["tp"]

    def program(*args):
        heads = args[3].shape[1] // tp
        exp_dev = args[9].shape[0] // sp
        deals = sp % 2 == 0 and heads * 2 == sp and exp_dev == tp and tp == 4
        body = layer if deals else generic_shards
        mapped = jax.shard_map(body, mesh=mesh, in_specs=placed, out_specs=P("sp", "tp"), check_vma=False)
        return mapped(*args)

    return program
```
